32 devices in a mesh: grp: 2 (over x), sp: 4 (over y, core), tp: 4 (over z).
Axes of the slice: x: 2, y: 2, z: 4, core: 2. Of those that a mesh axis runs over, the one named last changes fastest.
Arguments:
- tokens: bfloat16 [8, 1024, 2048], P(('grp', 'tp'), 'sp'), parts along dimension 0, may hold values from -6 to 6
- kv_down: bfloat16 [2048, 512], replicated, may hold values from -0.125 to 0.125
- rope_down: bfloat16 [2048, 64], replicated, may hold values from -0.125 to 0.125
- kv_gain: float32 [512], replicated, may hold values from 0.1 to 1.9
- key_up: bfloat16 [512, 16, 128], replicated, may hold values from -0.25 to 0.25
- value_up: bfloat16 [512, 16, 128], replicated, may hold values from -0.25 to 0.25
- query_nope: bfloat16 [8, 16, 128], P(('grp', 'sp'), 'tp'), parts along dimension 0, may hold values from -180 to 180
- query_rope: bfloat16 [8, 16, 64], P(('grp', 'sp'), 'tp'), parts along dimension 0, may hold values from -180 to 180
Outputs:
- key_cache: bfloat16 [8, 16, 1024, 128], P(('grp', 'sp'), 'tp'), parts along dimension 0
- value_cache: bfloat16 [8, 16, 1024, 128], P(('grp', 'sp'), 'tp'), parts along dimension 0
- rope_cache: bfloat16 [8, 1024, 64], P(('grp', 'sp')), parts along dimension 0
- read_out: bfloat16 [8, 16, 128], P(('grp', 'sp'), 'tp'), parts along dimension 0
The draws below stay inside these ranges and needn't reach their ends.
There are 2 independent parts, one for each index of `grp`. The reference program is written for one: setup_inputs(seed, part) draws one part's arguments, and reference() takes and returns one part's arrays. A program takes and returns all parts, laid end to end along the dimension named above; an argument that names none is the same for every part. Nothing has to cross between parts.
All inputs are finite; a program needn't handle non-finite values.
Results may differ from the reference program's by a relative error of at most 0.018.
The reference program's roundings to bfloat16 on the way (of `normed` and `rotated`) count: a program that leaves them out, or rounds other values in their place, can miss the bound.
Values may be sent and summed in bfloat16 or wider, within the bound.
A program may use at most 64 MiB of HBM per device.

```python
import jax
import jax.numpy as jnp
from jax import lax

D = 2048
HEADS = 16
KVL = 512
NOPE = 128
ROPE = 64
VD = 128
SEQS = 4
LEN = 1024


def query_draw(key, width):
    base = jax.random.normal(jax.random.fold_in(key, 11), (SEQS, HEADS, width), jnp.float32)
    base = jnp.clip(base, -6.0, 6.0)
    return base.astype(jnp.bfloat16)


def draw_query_nope(key, part):
    return query_draw(jax.random.fold_in(key, 1), NOPE)


def draw_query_rope(key, part):
    return query_draw(jax.random.fold_in(key, 2), ROPE)


def steps_of(key, shape, shards, least, high):
    loudness = 1.0
    for dim, blocks in shards:
        heights = jax.random.uniform(jax.random.fold_in(jax.random.fold_in(key, 6), dim), (blocks,), jnp.float32, least / len(shards), high / len(shards))
        loudness = loudness * jnp.repeat(jnp.exp(heights), shape[dim] // blocks).reshape((-1,) + (1,) * (len(shape) - 1 - dim))
    return loudness


def noise(stream_key, shape, scale, limit, pieces=(), kind=jnp.bfloat16):
    values = scale * jax.random.normal(stream_key, shape, jnp.float32)
    if pieces:
        values = values * steps_of(stream_key, shape, pieces, -0.22, 0.18)
    return jnp.clip(values, -limit, limit).astype(kind)


def setup_inputs(seed: int = 0, part: int = 0) -> dict:
    arg_keys = jax.random.split(jax.random.key(seed), 9)
    part_keys = jax.random.split(jax.random.fold_in(arg_keys[8], part), 9)
    return {
        "tokens": noise(part_keys[0], (SEQS, LEN, D), 1.0, 6.0, ((0, 4), (1, 4))),
        "kv_down": noise(arg_keys[1], (D, KVL), D ** -0.5, 0.125),
        "rope_down": noise(arg_keys[2], (D, ROPE), D ** -0.5, 0.125),
        "kv_gain": jnp.clip(1.0 + 0.18 * jax.random.normal(arg_keys[3], (KVL,), jnp.float32), 0.1, 1.9),
        "key_up": noise(arg_keys[4], (KVL, HEADS, NOPE), KVL ** -0.5, 0.25),
        "value_up": noise(arg_keys[5], (KVL, HEADS, VD), KVL ** -0.5, 0.25),
        "query_nope": draw_query_nope(jax.random.fold_in(jax.random.fold_in(arg_keys[8], part), 71), part),
        "query_rope": draw_query_rope(jax.random.fold_in(jax.random.fold_in(arg_keys[8], part), 71), part),
    }


norm_epsilon = 1e-06
rope_base = 10000.0

def rotate(values, positions):
    half_width = values.shape[-1] // 2
    frequency = 1.0 / rope_base ** (jnp.arange(0, 2 * half_width, 2, dtype=jnp.float32) / (2 * half_width))
    angles = positions[..., None] * frequency
    cosine = jnp.cos(angles)
    sine_part = jnp.sin(angles)
    front_half = values[..., :half_width]
    back_half = values[..., half_width:]
    return jnp.concatenate([front_half * cosine - back_half * sine_part, front_half * sine_part + back_half * cosine], axis=-1)

def reference(tokens, kv_down, rope_down, kv_gain, key_up, value_up, query_nope, query_rope):
    positions = jnp.arange(LEN, dtype=jnp.float32)
    key_flat = key_up.reshape(KVL, HEADS * NOPE)
    value_flat = value_up.reshape(KVL, HEADS * VD)

    def one_sequence(seq_rows):
        latent = jnp.dot(seq_rows, kv_down, preferred_element_type=jnp.float32)
        normed = (latent * lax.rsqrt(lax.optimization_barrier(jnp.mean(latent * latent, axis=-1, keepdims=True)) + norm_epsilon) * kv_gain).astype(jnp.bfloat16)
        rope_raw = jnp.dot(seq_rows, rope_down, preferred_element_type=jnp.float32)
        rope_key = rotate(rope_raw, positions).astype(jnp.bfloat16)
        key_rows = jnp.dot(normed, key_flat, preferred_element_type=jnp.float32).astype(jnp.bfloat16)
        value_rows = jnp.dot(normed, value_flat, preferred_element_type=jnp.float32).astype(jnp.bfloat16)
        key_rows = key_rows.reshape(LEN, HEADS, NOPE).transpose(1, 0, 2)
        value_rows = value_rows.reshape(LEN, HEADS, VD).transpose(1, 0, 2)
        return (key_rows, value_rows, rope_key)
    key_cache, value_cache, rope_cache = lax.map(one_sequence, tokens)
    query_pos = jnp.full((HEADS,), LEN, dtype=jnp.float32)
    rotated = rotate(query_rope.astype(jnp.float32), query_pos).astype(jnp.bfloat16)
    score_scale = (NOPE + ROPE) ** (-0.5)
    scores = jnp.einsum('shd,shld->shl', query_nope.astype(jnp.float32), key_cache.astype(jnp.float32))
    scores = scores + jnp.einsum('shr,slr->shl', rotated.astype(jnp.float32), rope_cache.astype(jnp.float32))
    scores = scores * score_scale
    row_max = lax.optimization_barrier(jnp.max(scores, axis=-1, keepdims=True))
    expo_terms = jnp.exp(scores - row_max)
    weights = expo_terms / lax.optimization_barrier(jnp.sum(expo_terms, axis=-1, keepdims=True))
    read_out = jnp.einsum('shl,shld->shd', weights, value_cache.astype(jnp.float32)).astype(jnp.bfloat16)
    return (key_cache, value_cache, rope_cache, read_out)
```

```python
import functools

import jax
import jax.numpy as jnp
import numpy as np
from jax import lax
from jax.experimental import pallas as pl
from jax.experimental.pallas import tpu as pltpu
from jax.sharding import PartitionSpec as P

norm_epsilon = 1e-06
rope_base = 10000.0
MESH = pl.DeviceIdType.MESH
F32, BF16 = jnp.float32, jnp.bfloat16


def tables(length, width):
    frequency = (1.0 / rope_base ** (np.arange(0, width, 2, dtype=np.float64) / width)).astype(np.float32)
    angles = frequency[:, None] * np.arange(length, dtype=np.float32)[None, :]
    cached = np.stack([np.cos(angles.astype(np.float64)), np.sin(angles.astype(np.float64))])
    ask = (np.float32(length) * frequency).astype(np.float64)
    asked = np.stack([np.tile(np.cos(ask), 2), np.tile(np.sin(ask), 2)])
    return cached.astype(np.float32), asked.astype(np.float32)


def kernel(
    sp_count, tp_count, bounds, scale,
    tok, kvd, rpt, gain, kup, vup, qn, qr, tab, qtab,
    key_out, val_out, rope_out, read_out,
    box, tok_v, kvd_v, rpt_v, gain_v, up_v, wide, kw, vw, qn_v, qr_v, tab_v, qtab_v, scores,
    in_sem, zsend, zrecv, csend, crecv,
):
    me = lax.axis_index("sp")
    here = lax.axis_index("tp")
    seq_local, pos_dev, _ = tok.shape
    rope_width = rpt.shape[0]
    half = rope_width // 2
    heads_dev, key_width = qn.shape[1], qn.shape[2]
    rope_rows = bounds[0]
    pieces = [pl.ds(a, b - a) for a, b in zip((0,) + bounds[1:-1], bounds[1:])]
    count = len(pieces)
    last = tp_count - 1

    barrier = pltpu.get_barrier_semaphore()
    for step in range(1, sp_count):
        pl.semaphore_signal(
            barrier, inc=1, device_id={"sp": lax.rem(me + step, sp_count)}, device_id_type=MESH
        )
    if tp_count > 1:
        for step in (1, last):
            pl.semaphore_signal(
                barrier, inc=1, device_id={"tp": lax.rem(here + step, tp_count)}, device_id_type=MESH
            )

    tile = up_v.shape[2]
    head_start = here * heads_dev
    head_tile = pl.multiple_of(head_start // tile * tile, tile)
    head_off = lax.rem(head_start, tile)
    loads = [
        pltpu.make_async_copy(src, dst, in_sem.at[n])
        for n, (src, dst) in enumerate([
            (tok, tok_v),
            (kvd, kvd_v),
            (gain, gain_v),
            (rpt, rpt_v),
            (tab.at[:, :, pl.ds(pl.multiple_of(me * pos_dev, pos_dev), pos_dev)], tab_v),
            (kup.at[:, pl.ds(head_tile, tile), :], up_v.at[0]),
            (vup.at[:, pl.ds(head_tile, tile), :], up_v.at[1]),
            (qn, qn_v),
            (qr, qr_v),
            (qtab, qtab_v),
        ])
    ]
    for load in loads:
        load.start()

    def slot(prompt):
        return jnp.where(prompt == me, me, sp_count + prompt)

    for n in (3, 4, 0):
        loads[n].wait()
    for q in range(seq_local):
        mine = slot(here * seq_local + q)
        rows = tok_v[q]
        raw = lax.dot_general(rpt_v[...], rows, (((1,), (1,)), ((), ())), preferred_element_type=F32)
        cosine, sine_part = tab_v[0], tab_v[1]
        front, back = raw[:half], raw[half:]
        turned = jnp.concatenate(
            [front * cosine - back * sine_part, front * sine_part + back * cosine], axis=0
        ).astype(BF16)
        groups = rope_width // rope_rows
        box[mine, 0:rope_rows, :] = jnp.concatenate(
            [turned[g * rope_rows:(g + 1) * rope_rows] for g in range(groups)], axis=1
        )
    for n in (1, 2):
        loads[n].wait()
    for q in range(seq_local):
        mine = slot(here * seq_local + q)
        latent = jnp.dot(tok_v[q], kvd_v[...], preferred_element_type=F32)
        normed = (
            latent
            * lax.rsqrt(jnp.mean(latent * latent, axis=-1, keepdims=True) + norm_epsilon)
            * gain_v[...]
        ).astype(BF16)
        box[mine, rope_rows:rope_rows + pos_dev, :] = normed

    def along(prompt, way, hop, q, s):
        part = box.at[slot(prompt), pieces[s]]
        return pltpu.make_async_remote_copy(
            src_ref=part, dst_ref=part,
            send_sem=zsend.at[way, hop, q, s], recv_sem=zrecv.at[way, hop, q, s],
            device_id={"tp": here + (1 if way == 0 else -1)}, device_id_type=MESH,
        )

    def across(prompt, s):
        return pltpu.make_async_remote_copy(
            src_ref=box.at[slot(prompt), pieces[s]], dst_ref=box.at[me, pieces[s]],
            send_sem=csend.at[prompt, s], recv_sem=crecv.at[me, s],
            device_id={"sp": prompt}, device_id_type=MESH,
        )

    pl.semaphore_wait(barrier, sp_count - 1 + (2 if tp_count > 1 else 0))
    inner = {0: here < last, 1: here > 0}
    for q in range(seq_local):
        prompt = here * seq_local + q
        for s in range(count):
            for way in (0, 1):
                @pl.when(inner[way])
                def _(way=way, s=s):
                    along(prompt, way, 0, q, s).start()

            @pl.when(prompt != me)
            def _(s=s):
                across(prompt, s).start()

    for n in (5, 6, 7, 8, 9):
        loads[n].wait()
    depth = up_v.shape[1]
    for n, target in enumerate((kw, vw)):
        wide[...] = up_v[n].astype(F32).reshape(depth * tile, key_width)
        for h in range(heads_dev):
            target[:, h * key_width:(h + 1) * key_width] = wide[
                pl.ds(head_off + h, depth, stride=tile), :
            ].astype(BF16)

    for hop in range(last):
        for q in range(seq_local):
            for s in range(count):
                for way in (0, 1):
                    owner = here - 1 - hop if way == 0 else here + 1 + hop
                    has = owner >= 0 if way == 0 else owner <= last

                    @pl.when(has)
                    def _(way=way, s=s, owner=owner):
                        prompt = owner * seq_local + q
                        along(prompt, way, hop, q, s).wait_recv()
                        if hop + 1 < last:
                            @pl.when(inner[way])
                            def _():
                                along(prompt, way, hop + 1, q, s).start()

                        @pl.when(prompt != me)
                        def _():
                            across(prompt, s).start()

    query = qn_v[0]
    zero = jnp.zeros_like(query)
    picks = lax.broadcasted_iota(jnp.int32, query.shape, 0)
    spread = jnp.concatenate(
        [jnp.where(picks == h, query.astype(F32), zero.astype(F32)) for h in range(heads_dev)], axis=1
    ).astype(BF16)
    ask = qr_v[0].astype(F32)
    swapped = jnp.concatenate([-ask[:, half:], ask[:, :half]], axis=1)
    rotated = (ask * qtab_v[0:1, :] + swapped * qtab_v[1:2, :]).astype(BF16)
    group_rows = pos_dev // 2
    for group in range(2):
        for step in range(sp_count):
            source = lax.rem(me + step, sp_count)
            if step:
                for s in ((0,) if group == 0 else range(1, count)):
                    part = box.at[source, pieces[s]]
                    pltpu.make_async_remote_copy(
                        src_ref=part, dst_ref=part,
                        send_sem=csend.at[source, s], recv_sem=crecv.at[source, s],
                        device_id={"sp": source}, device_id_type=MESH,
                    ).wait_recv()
            block = pl.ds(pl.multiple_of(source * pos_dev, pos_dev), pos_dev)
            if group == 0:
                packed = box[source, 0:rope_rows, :]
                turned = jnp.concatenate(
                    [packed[:, g * pos_dev:(g + 1) * pos_dev] for g in range(rope_width // rope_rows)], axis=0
                )
                rope_out[0, :, block] = turned
            begin = rope_rows + group * group_rows
            rows = box[source, begin:begin + group_rows, :]
            place = pl.ds(pl.multiple_of(source * pos_dev + group * group_rows, group_rows), group_rows)
            keys = jnp.dot(rows, kw[...], preferred_element_type=F32).astype(BF16)
            values = jnp.dot(rows, vw[...], preferred_element_type=F32).astype(BF16)
            for h in range(heads_dev):
                key_out[0, h, place, :] = keys[:, h * key_width:(h + 1) * key_width]
                val_out[0, h, place, :] = values[:, h * key_width:(h + 1) * key_width]
            scores[:, place] = lax.dot_general(
                spread, keys, (((1,), (1,)), ((), ())), preferred_element_type=F32
            )

    total = scores[...] + jnp.dot(rotated, rope_out[0], preferred_element_type=F32)
    total = total * scale
    terms = jnp.exp(total - jnp.max(total, axis=-1, keepdims=True))
    weights = terms / jnp.sum(terms, axis=-1, keepdims=True)
    high = weights.astype(BF16)
    low = (weights - high.astype(F32)).astype(BF16)
    both = jnp.concatenate([high.astype(F32), low.astype(F32)], axis=0).astype(BF16)
    reads = []
    for h in range(heads_dev):
        read = jnp.dot(both, val_out[0, h], preferred_element_type=F32)
        reads.append(read[h:h + 1] + read[heads_dev + h:heads_dev + h + 1])
    read_out[0] = jnp.concatenate(reads, axis=0).astype(BF16)

    for hop in range(last):
        for q in range(seq_local):
            for s in range(count):
                for way in (0, 1):
                    owner = here - hop if way == 0 else here + hop
                    has = owner >= 0 if way == 0 else owner <= last

                    @pl.when(jnp.logical_and(has, inner[way]))
                    def _(way=way, s=s, owner=owner):
                        along(owner * seq_local + q, way, hop, q, s).wait_send()
    for step in range(1, sp_count):
        prompt = lax.rem(me + step, sp_count)
        for s in range(count):
            across(prompt, s).wait_send()


def local(tokens, kv_down, rope_down, kv_gain, key_up, value_up, query_nope, query_rope):
    seq_local, pos_dev, model_width = tokens.shape
    sp_count = lax.axis_size("sp")
    tp_count = lax.axis_size("tp")
    latent_width = kv_down.shape[1]
    rope_width = rope_down.shape[1]
    head_count, key_width = key_up.shape[1], key_up.shape[2]
    heads_dev = head_count // tp_count
    length = pos_dev * sp_count
    rope_rows = rope_width * pos_dev // latent_width
    rows = rope_rows + pos_dev
    bounds = (rope_rows, rope_rows + pos_dev // 2, rope_rows + pos_dev * 3 // 4, rows)
    prompts = tp_count * seq_local
    cached, asked = tables(length, rope_width)
    tile = 8
    any_space = pl.BlockSpec(memory_space=pl.ANY)
    vmem = pl.BlockSpec(memory_space=pltpu.VMEM)
    hops = max(tp_count - 1, 1)
    count = len(bounds) - 1
    dma = pltpu.SemaphoreType.DMA
    key_cache, value_cache, rope_t, read_out = pl.pallas_call(
        functools.partial(kernel, sp_count, tp_count, bounds, (key_width + rope_width) ** (-0.5)),
        out_shape=(
            jax.ShapeDtypeStruct((1, heads_dev, length, key_width), BF16),
            jax.ShapeDtypeStruct((1, heads_dev, length, key_width), BF16),
            jax.ShapeDtypeStruct((1, rope_width, length), BF16),
            jax.ShapeDtypeStruct((1, heads_dev, key_width), BF16),
        ),
        in_specs=[any_space] * 10,
        out_specs=(vmem,) * 4,
        scratch_shapes=[
            pltpu.VMEM((sp_count + prompts, rows, latent_width), BF16),
            pltpu.VMEM(tokens.shape, BF16),
            pltpu.VMEM(kv_down.shape, BF16),
            pltpu.VMEM((rope_width, model_width), BF16),
            pltpu.VMEM((1, latent_width), F32),
            pltpu.VMEM((2, latent_width, tile, key_width), BF16),
            pltpu.VMEM((latent_width * tile, key_width), F32),
            pltpu.VMEM((latent_width, heads_dev * key_width), BF16),
            pltpu.VMEM((latent_width, heads_dev * key_width), BF16),
            pltpu.VMEM(query_nope.shape, BF16),
            pltpu.VMEM(query_rope.shape, BF16),
            pltpu.VMEM((2, rope_width // 2, pos_dev), F32),
            pltpu.VMEM((2, rope_width), F32),
            pltpu.VMEM((heads_dev, length), F32),
            dma((10,)),
            dma((2, hops, seq_local, count)),
            dma((2, hops, seq_local, count)),
            dma((prompts, count)),
            dma((sp_count, count)),
        ],
        compiler_params=pltpu.CompilerParams(
            collective_id=0, has_side_effects=True, vmem_limit_bytes=40 * 1024 * 1024
        ),
    )(
        tokens, kv_down, rope_down.T, kv_gain.reshape(1, latent_width), key_up, value_up,
        query_nope, query_rope, jnp.asarray(cached), jnp.asarray(asked),
    )
    return (key_cache, value_cache, jnp.swapaxes(rope_t, 1, 2), read_out)


def solution(mesh):
    placed = (
        P(("grp", "tp"), "sp", None),
        P(),
        P(),
        P(),
        P(),
        P(),
        P(("grp", "sp"), "tp", None),
        P(("grp", "sp"), "tp", None),
    )
    return jax.shard_map(
        local,
        mesh=mesh,
        in_specs=placed,
        out_specs=(
            P(("grp", "sp"), "tp", None, None),
            P(("grp", "sp"), "tp", None, None),
            P(("grp", "sp"), None, None),
            P(("grp", "sp"), "tp", None),
        ),
        check_vma=False,
    )
```

```python
import functools

import jax
import jax.numpy as jnp
import numpy as np
from jax import lax
from jax.experimental import pallas as pl
from jax.experimental.pallas import tpu as pltpu
from jax.sharding import PartitionSpec as P

norm_epsilon = 1e-06
rope_base = 10000.0
MESH = pl.DeviceIdType.MESH
F32, BF16 = jnp.float32, jnp.bfloat16


def tables(length, width):
    frequency = (1.0 / rope_base ** (np.arange(0, width, 2, dtype=np.float64) / width)).astype(np.float32)
    angles = frequency[:, None] * np.arange(length, dtype=np.float32)[None, :]
    cached = np.stack([np.cos(angles.astype(np.float64)), np.sin(angles.astype(np.float64))])
    ask = (np.float32(length) * frequency).astype(np.float64)
    asked = np.stack([np.tile(np.cos(ask), 2), np.tile(np.sin(ask), 2)])
    return cached.astype(np.float32), asked.astype(np.float32)


def kernel(
    sp_count, tp_count, heads_dev, bounds,
    tok, kvd, rpt, gain, kup, vup, tab,
    key_out, val_out, rope_out,
    box, tok_v, kvd_v, rpt_v, gain_v, up_v, wide, kw, vw, tab_v,
    in_sem, zsend, zrecv, csend, crecv,
):
    me = lax.axis_index("sp")
    here = lax.axis_index("tp")
    seq_local, pos_dev, _ = tok.shape
    rope_width = rpt.shape[0]
    half = rope_width // 2
    key_width = kup.shape[2]
    rope_rows = bounds[0]
    pieces = [pl.ds(a, b - a) for a, b in zip((0,) + bounds[1:-1], bounds[1:])]
    count = len(pieces)
    last = tp_count - 1

    barrier = pltpu.get_barrier_semaphore()
    for step in range(1, sp_count):
        pl.semaphore_signal(
            barrier, inc=1, device_id={"sp": lax.rem(me + step, sp_count)}, device_id_type=MESH
        )
    if tp_count > 1:
        for step in (1, last):
            pl.semaphore_signal(
                barrier, inc=1, device_id={"tp": lax.rem(here + step, tp_count)}, device_id_type=MESH
            )

    tile = up_v.shape[2]
    head_start = here * heads_dev
    head_tile = pl.multiple_of(head_start // tile * tile, tile)
    head_off = lax.rem(head_start, tile)
    loads = [
        pltpu.make_async_copy(src, dst, in_sem.at[n])
        for n, (src, dst) in enumerate([
            (tok, tok_v),
            (kvd, kvd_v),
            (gain, gain_v),
            (rpt, rpt_v),
            (tab.at[:, :, pl.ds(pl.multiple_of(me * pos_dev, pos_dev), pos_dev)], tab_v),
            (kup.at[:, pl.ds(head_tile, tile), :], up_v.at[0]),
            (vup.at[:, pl.ds(head_tile, tile), :], up_v.at[1]),
        ])
    ]
    for load in loads:
        load.start()

    def slot(prompt):
        return jnp.where(prompt == me, me, sp_count + prompt)

    for n in (3, 4, 0):
        loads[n].wait()
    for q in range(seq_local):
        mine = slot(here * seq_local + q)
        rows = tok_v[q]
        raw = lax.dot_general(rpt_v[...], rows, (((1,), (1,)), ((), ())), preferred_element_type=F32)
        cosine, sine_part = tab_v[0], tab_v[1]
        front, back = raw[:half], raw[half:]
        turned = jnp.concatenate(
            [front * cosine - back * sine_part, front * sine_part + back * cosine], axis=0
        ).astype(BF16)
        groups = rope_width // rope_rows
        box[mine, 0:rope_rows, :] = jnp.concatenate(
            [turned[g * rope_rows:(g + 1) * rope_rows] for g in range(groups)], axis=1
        )
    def along(prompt, way, hop, q, s):
        part = box.at[slot(prompt), pieces[s]]
        return pltpu.make_async_remote_copy(
            src_ref=part, dst_ref=part,
            send_sem=zsend.at[way, hop, q, s], recv_sem=zrecv.at[way, hop, q, s],
            device_id={"tp": here + (1 if way == 0 else -1)}, device_id_type=MESH,
        )

    def across(prompt, s):
        return pltpu.make_async_remote_copy(
            src_ref=box.at[slot(prompt), pieces[s]], dst_ref=box.at[me, pieces[s]],
            send_sem=csend.at[prompt, s], recv_sem=crecv.at[me, s],
            device_id={"sp": prompt}, device_id_type=MESH,
        )

    inner = {0: here < last, 1: here > 0}
    for n in (1, 2):
        loads[n].wait()
    half_rows = pos_dev // 2
    for group in range(2):
        for q in range(seq_local):
            mine = slot(here * seq_local + q)
            latent = jnp.dot(
                tok_v[q, group * half_rows:(group + 1) * half_rows, :], kvd_v[...],
                preferred_element_type=F32,
            )
            normed = (
                latent
                * lax.rsqrt(jnp.mean(latent * latent, axis=-1, keepdims=True) + norm_epsilon)
                * gain_v[...]
            ).astype(BF16)
            begin = rope_rows + group * half_rows
            box[mine, begin:begin + half_rows, :] = normed
        if group == 0:
            pl.semaphore_wait(barrier, sp_count - 1 + (2 if tp_count > 1 else 0))
        for q in range(seq_local):
            prompt = here * seq_local + q
            for s in ((0,) if group == 0 else range(1, count)):
                for way in (0, 1):
                    @pl.when(inner[way])
                    def _(way=way, s=s):
                        along(prompt, way, 0, q, s).start()

                @pl.when(prompt != me)
                def _(s=s):
                    across(prompt, s).start()

    for n in (5, 6):
        loads[n].wait()
    depth = up_v.shape[1]
    for n, target in enumerate((kw, vw)):
        wide[...] = up_v[n].astype(F32).reshape(depth * tile, key_width)
        for h in range(heads_dev):
            target[:, h * key_width:(h + 1) * key_width] = wide[
                pl.ds(head_off + h, depth, stride=tile), :
            ].astype(BF16)

    for hop in range(last):
        for q in range(seq_local):
            for s in range(count):
                for way in (0, 1):
                    owner = here - 1 - hop if way == 0 else here + 1 + hop
                    has = owner >= 0 if way == 0 else owner <= last

                    @pl.when(has)
                    def _(way=way, s=s, owner=owner):
                        prompt = owner * seq_local + q
                        along(prompt, way, hop, q, s).wait_recv()
                        if hop + 1 < last:
                            @pl.when(inner[way])
                            def _():
                                along(prompt, way, hop + 1, q, s).start()

                        @pl.when(prompt != me)
                        def _():
                            across(prompt, s).start()

    group_rows = pos_dev // 2
    for group in range(2):
        for step in range(sp_count):
            source = lax.rem(me + step, sp_count)
            if step:
                for s in ((0,) if group == 0 else range(1, count)):
                    part = box.at[source, pieces[s]]
                    pltpu.make_async_remote_copy(
                        src_ref=part, dst_ref=part,
                        send_sem=csend.at[source, s], recv_sem=crecv.at[source, s],
                        device_id={"sp": source}, device_id_type=MESH,
                    ).wait_recv()
            block = pl.ds(pl.multiple_of(source * pos_dev, pos_dev), pos_dev)
            if group == 0:
                packed = box[source, 0:rope_rows, :]
                turned = jnp.concatenate(
                    [packed[:, g * pos_dev:(g + 1) * pos_dev] for g in range(rope_width // rope_rows)], axis=0
                )
                rope_out[0, :, block] = turned
            begin = rope_rows + group * group_rows
            rows = box[source, begin:begin + group_rows, :]
            place = pl.ds(pl.multiple_of(source * pos_dev + group * group_rows, group_rows), group_rows)
            keys = jnp.dot(rows, kw[...], preferred_element_type=F32).astype(BF16)
            values = jnp.dot(rows, vw[...], preferred_element_type=F32).astype(BF16)
            for h in range(heads_dev):
                key_out[0, h, place, :] = keys[:, h * key_width:(h + 1) * key_width]
                val_out[0, h, place, :] = values[:, h * key_width:(h + 1) * key_width]

    for hop in range(last):
        for q in range(seq_local):
            for s in range(count):
                for way in (0, 1):
                    owner = here - hop if way == 0 else here + hop
                    has = owner >= 0 if way == 0 else owner <= last

                    @pl.when(jnp.logical_and(has, inner[way]))
                    def _(way=way, s=s, owner=owner):
                        along(owner * seq_local + q, way, hop, q, s).wait_send()
    for step in range(1, sp_count):
        prompt = lax.rem(me + step, sp_count)
        for s in range(count):
            across(prompt, s).wait_send()


def finish(scale, keys, vals, ropes, query, ask, qtab, key_out, val_out, rope_out, read_out, sem):
    moves = [
        pltpu.make_async_copy(src, dst, sem.at[n])
        for n, (src, dst) in enumerate([(vals, val_out), (keys, key_out), (ropes, rope_out)])
    ]
    for move in moves:
        move.start()
    heads_dev = query.shape[1]
    half = ask.shape[2] // 2
    turn = ask[0].astype(F32)
    swapped = jnp.concatenate([-turn[:, half:], turn[:, :half]], axis=1)
    rotated = (turn * qtab[0:1, :] + swapped * qtab[1:2, :]).astype(BF16)
    asked = query[0]
    picks = []
    for h in range(heads_dev):
        full = lax.dot_general(
            asked, keys[0, h], (((1,), (1,)), ((), ())), preferred_element_type=F32
        )
        picks.append(full[h:h + 1])
    total = jnp.concatenate(picks, axis=0)
    total = (total + jnp.dot(rotated, ropes[0], preferred_element_type=F32)) * scale
    terms = jnp.exp(total - jnp.max(total, axis=-1, keepdims=True))
    weights = terms / jnp.sum(terms, axis=-1, keepdims=True)
    high = weights.astype(BF16).astype(F32)
    both = jnp.concatenate([high, weights - high], axis=0).astype(BF16)
    reads = []
    for h in range(heads_dev):
        read = jnp.dot(both, vals[0, h], preferred_element_type=F32)
        reads.append(read[h:h + 1] + read[heads_dev + h:heads_dev + h + 1])
    read_out[0] = jnp.concatenate(reads, axis=0).astype(BF16)
    for move in moves:
        move.wait()


def local(tokens, kv_down, rope_down, kv_gain, key_up, value_up, query_nope, query_rope):
    seq_local, pos_dev, model_width = tokens.shape
    sp_count = lax.axis_size("sp")
    tp_count = lax.axis_size("tp")
    latent_width = kv_down.shape[1]
    rope_width = rope_down.shape[1]
    head_count, key_width = key_up.shape[1], key_up.shape[2]
    heads_dev = head_count // tp_count
    length = pos_dev * sp_count
    rope_rows = rope_width * pos_dev // latent_width
    rows = rope_rows + pos_dev
    bounds = (rope_rows, rope_rows + pos_dev // 2, rope_rows + pos_dev * 3 // 4, rows)
    prompts = tp_count * seq_local
    cached, asked = tables(length, rope_width)
    tile = 8
    any_space = pl.BlockSpec(memory_space=pl.ANY)
    vmem = pl.BlockSpec(memory_space=pltpu.VMEM)
    hops = max(tp_count - 1, 1)
    count = len(bounds) - 1
    dma = pltpu.SemaphoreType.DMA
    parts = pl.pallas_call(
        functools.partial(kernel, sp_count, tp_count, heads_dev, bounds),
        out_shape=(
            jax.ShapeDtypeStruct((1, heads_dev, length, key_width), BF16),
            jax.ShapeDtypeStruct((1, heads_dev, length, key_width), BF16),
            jax.ShapeDtypeStruct((1, rope_width, length), BF16),
        ),
        in_specs=[any_space] * 7,
        out_specs=(vmem,) * 3,
        scratch_shapes=[
            pltpu.VMEM((sp_count + prompts, rows, latent_width), BF16),
            pltpu.VMEM(tokens.shape, BF16),
            pltpu.VMEM(kv_down.shape, BF16),
            pltpu.VMEM((rope_width, model_width), BF16),
            pltpu.VMEM((1, latent_width), F32),
            pltpu.VMEM((2, latent_width, tile, key_width), BF16),
            pltpu.VMEM((latent_width * tile, key_width), F32),
            pltpu.VMEM((latent_width, heads_dev * key_width), BF16),
            pltpu.VMEM((latent_width, heads_dev * key_width), BF16),
            pltpu.VMEM((2, rope_width // 2, pos_dev), F32),
            dma((7,)),
            dma((2, hops, seq_local, count)),
            dma((2, hops, seq_local, count)),
            dma((prompts, count)),
            dma((sp_count, count)),
        ],
        compiler_params=pltpu.CompilerParams(
            collective_id=0, has_side_effects=True, vmem_limit_bytes=53000000
        ),
    )(
        tokens, kv_down, rope_down.T, kv_gain.reshape(1, latent_width), key_up, value_up,
        jnp.asarray(cached),
    )
    key_cache, value_cache, rope_t, read_out = pl.pallas_call(
        functools.partial(finish, (key_width + rope_width) ** (-0.5)),
        out_shape=tuple(jax.ShapeDtypeStruct(part.shape, BF16) for part in parts)
        + (jax.ShapeDtypeStruct((1, heads_dev, key_width), BF16),),
        in_specs=[vmem] * 6,
        out_specs=(any_space,) * 3 + (vmem,),
        scratch_shapes=[dma((3,))],
        compiler_params=pltpu.CompilerParams(vmem_limit_bytes=8 * 1024 * 1024),
    )(*parts, query_nope, query_rope, jnp.asarray(asked))
    return (key_cache, value_cache, jnp.swapaxes(rope_t, 1, 2), read_out)


def solution(mesh):
    placed = (
        P(("grp", "tp"), "sp", None),
        P(),
        P(),
        P(),
        P(),
        P(),
        P(("grp", "sp"), "tp", None),
        P(("grp", "sp"), "tp", None),
    )
    return jax.shard_map(
        local,
        mesh=mesh,
        in_specs=placed,
        out_specs=(
            P(("grp", "sp"), "tp", None, None),
            P(("grp", "sp"), "tp", None, None),
            P(("grp", "sp"), None, None),
            P(("grp", "sp"), "tp", None),
        ),
        check_vma=False,
    )
```
